32 devices in a mesh: grp: 2 (over x), ep: 16 (over z, y, core), tp: 1.
Axes of the slice: x: 2, y: 2, z: 4, core: 2. Of those that a mesh axis runs over, the one named last changes fastest.
Arguments:
- tokens: bfloat16 [2048, 1024], P(('grp', 'ep')), parts along dimension 0, may hold values from -6 to 6
- norm_gain: float32 [1024], replicated, may hold values from 0.1 to 1.9
- routes: int32 [2048, 6], P(('grp', 'ep')), parts along dimension 0, may hold values from 0 to 15, all different within a row; in each aligned block of 64 rows (0 to 63, 64 to 127, ...) at most 32 rows name the same one
- gate_weights: float32 [2048, 6], P(('grp', 'ep')), parts along dimension 0, may hold values from 0.1 to 1
- w_gate: bfloat16 [16, 1024, 2048], P('ep', None, 'tp'), may hold values from -0.1875 to 0.1875
- w_up: bfloat16 [16, 1024, 2048], P('ep', None, 'tp'), may hold values from -0.1875 to 0.1875
- w_down: bfloat16 [16, 2048, 1024], P('ep', 'tp'), may hold values from -0.125 to 0.125
Outputs:
- mixed: bfloat16 [2048, 1024], P(('grp', 'ep')), parts along dimension 0
The draws below stay inside these ranges and needn't reach their ends.
There are 2 independent parts, one for each index of `grp`. The reference program is written for one: setup_inputs(seed, part) draws one part's arguments, and reference() takes and returns one part's arrays. A program takes and returns all parts, laid end to end along the dimension named above; an argument that names none is the same for every part. Nothing has to cross between parts.
Inputs may be any that keep to these rules, and one draw needn't show every extreme that they name: `routes`: each row names 6 different experts. Within the rows of one index of ep no expert is named more than 32 times, and in every draw some expert is named exactly 32 times in some index's rows.
All inputs are finite; a program needn't handle non-finite values.
Results may differ from the reference program's by a relative error of at most 0.013.
Values may be sent and summed in bfloat16 or wider, within the bound.
A program may use at most 64 MiB of HBM per device.

```python
import math
import jax
import jax.numpy as jnp
import numpy as np
from jax import lax

D = 1024
FF = 2048
TOPK = 6
TOK_DEV = 64
EXPERTS = 16
CAP = 32
TOKENS = 1024
N_EP = 16
N_TP = 1


def levels(own_key, extent, shards, smallest, high):
    def one(position, parts):
        steps = jax.random.uniform(jax.random.fold_in(jax.random.fold_in(own_key, 6), position), (parts,), jnp.float32, smallest / len(shards), high / len(shards))
        return jnp.repeat(jnp.exp(steps), extent[position] // parts).reshape((-1,) + (1,) * (len(extent) - position - 1))

    level = one(*shards[0])
    for cut in shards[1:]:
        level = level * one(*cut)
    return level


def deal_out(own_key, own, number, rows, count, top, reach, slope):
    ranking = jax.random.permutation(own_key, count)
    packed, usual = portions_of(count, rows * top, reach, slope, True), portions_of(count, rows * top, reach, slope, False)
    places = jnp.arange(count)

    def named(lengths, rotation):
        used = int((lengths > 0).sum())
        fixed = max(1, used // 4)
        passed = fixed + (places - fixed + rotation * (used - fixed)) % max(1, count - fixed)
        return jnp.zeros((count,), jnp.int32).at[ranking[jnp.where(places < fixed, places, passed)]].set(jnp.asarray(lengths, jnp.int32))

    lengths = jnp.where(number % 4 == 0, named(packed, number // 4), named(usual, number - number // 4 - 1))
    mixed = jax.random.permutation(jax.random.fold_in(own, 3), count)
    source_of, taker = mixed[0:count // 2 * 2:2], mixed[1:count // 2 * 2:2]
    room = jnp.minimum(lengths[source_of] - 1, reach - lengths[taker]) // 2
    room = jnp.where((source_of == ranking[0]) | (taker == ranking[0]) | (lengths[taker] == 0), 0, jnp.maximum(room, 0))
    passed = jax.random.randint(jax.random.fold_in(own, 4), (count // 2,), 0, 1 << 20) % (room + 1)
    lengths = lengths.at[source_of].add(-passed).at[taker].add(passed)
    members = jnp.searchsorted(jnp.cumsum(lengths), jnp.arange(rows * top), side="right").astype(jnp.int32)
    table = members.reshape(top, rows).T
    table = table[jax.random.permutation(jax.random.fold_in(own, 1), rows)]
    rotation = jax.random.randint(jax.random.fold_in(own, 2), (rows, 1), 0, top)
    return jnp.take_along_axis(table, (jnp.arange(top)[None, :] + rotation) % top, axis=1)


def portions_of(number_of, total, most, skew, full):
    loads = [(1 << 20) // math.isqrt(standing ** skew) + 1 for standing in range(1, number_of + 1)]
    largest = most if full else min(most, max(-(-total // number_of), total * loads[0] // sum(loads)))
    least = 1 if total - largest >= number_of - 1 else 0
    given, rest = [largest] + [least] * (number_of - 1), total - largest - least * (number_of - 1)
    while rest > 0:
        candidates = [i for i in range(1, number_of) if given[i] < largest] or [i for i in range(1, number_of) if given[i] < most]
        whole, left = sum([loads[i] for i in candidates]), rest
        for i in candidates:
            addition = min(most - given[i], max(1, left * loads[i] // whole), rest)
            given[i] = given[i] + addition
            rest = rest - addition
    return np.array(given)


def centred(rng, extent, width, limit, shards=(), kind=jnp.bfloat16):
    array = jax.random.normal(rng, extent, jnp.float32) * width
    if len(shards) > 0:
        array = levels(rng, extent, shards, -0.22, 0.18) * array
    return jnp.clip(array, min=-limit, max=limit).astype(kind)


def setup_inputs(seed: int = 0, part: int = 0) -> dict:
    key_of = jax.random.split(jax.random.key(seed), 8)
    part_keys = jax.random.split(jax.random.fold_in(key_of[7], part), 8)
    tokens = centred(part_keys[0], (TOKENS, D), 1.0, 6.0, ((0, 16),))
    norm_gain = jnp.clip(1.0 + 0.18 * jax.random.normal(key_of[1], (D,), jnp.float32), 0.1, 1.9)
    routes_keys = jax.random.split(jax.random.fold_in(part_keys[2], 1), TOKENS // TOK_DEV)
    routes_turns = jax.random.permutation(jax.random.fold_in(part_keys[2], 3), TOKENS // TOK_DEV)
    routes = jax.vmap(lambda own, number: deal_out(jax.random.fold_in(part_keys[2], 2), own, number, TOK_DEV, EXPERTS, TOPK, CAP, 2))(routes_keys, routes_turns).reshape((TOKENS, TOPK))
    gate_weights = jnp.clip(jnp.exp(math.log(1.0) - 2.3025851 * jax.random.uniform(part_keys[3], (TOKENS, TOPK), jnp.float32) ** levels(part_keys[3], (TOKENS, TOPK), ((0, 16),), -0.2, 0.2)), 0.1, 1.0)
    w_gate = centred(key_of[4], (EXPERTS, D, FF), D ** -0.5, 0.1875, ((0, 16),))
    w_up = centred(key_of[5], (EXPERTS, D, FF), D ** -0.5, 0.1875, ((0, 16),))
    w_down = centred(key_of[6], (EXPERTS, FF, D), FF ** -0.5, 0.125, ((0, 16),))
    return dict(tokens=tokens, norm_gain=norm_gain, routes=routes, gate_weights=gate_weights, w_gate=w_gate, w_up=w_up, w_down=w_down)


def reference(tokens, norm_gain, routes, gate_weights, w_gate, w_up, w_down):
    values = tokens.astype(jnp.float32)
    scale = lax.rsqrt(lax.optimization_barrier(jnp.mean(values * values, axis=-1, keepdims=True)) + 1e-06)
    normed = (values * scale * norm_gain).astype(jnp.bfloat16)
    half = FF // N_TP
    most = CAP * N_EP

    def serve(total, expert):
        match = routes == expert
        chosen = jnp.any(match, axis=1)
        weight = lax.optimization_barrier(jnp.sum(jnp.where(match, gate_weights, 0.0), axis=1))
        index = jnp.nonzero(chosen, size=most, fill_value=0)[0].astype(jnp.int32)
        valid = (jnp.arange(most, dtype=jnp.int32) < jnp.sum(chosen.astype(jnp.int32))).astype(jnp.float32)
        rows = normed[index]
        gate = jnp.dot(rows, w_gate[expert], preferred_element_type=jnp.float32)
        up = jnp.dot(rows, w_up[expert], preferred_element_type=jnp.float32)
        hidden = (jax.nn.silu(gate) * up).astype(jnp.bfloat16)
        summed = jnp.zeros((most, D), jnp.float32)
        for block in range(N_TP):
            partial_value = jnp.dot(hidden[:, block * half:(block + 1) * half], w_down[expert][block * half:(block + 1) * half], preferred_element_type=jnp.float32).astype(jnp.bfloat16)
            summed = summed + lax.optimization_barrier(partial_value).astype(jnp.float32)
        result = lax.optimization_barrier(summed.astype(jnp.bfloat16)).astype(jnp.float32)
        term = result * (weight[index] * valid)[:, None]
        return (total.at[index].add(term), None)
    total = jnp.zeros((tokens.shape[0], D), jnp.float32)
    total, _ = lax.scan(serve, total, jnp.arange(EXPERTS, dtype=jnp.int32))
    return total.astype(jnp.bfloat16)
```

```python
import functools

import jax
import jax.numpy as jnp
from jax import lax
from jax.experimental import pallas as pl
from jax.experimental.pallas import tpu as pltpu
from jax.sharding import PartitionSpec as P


def hidden_rows(rows, w_gate, w_up):
    gate = jnp.dot(rows, w_gate[0], preferred_element_type=jnp.float32)
    up = jnp.dot(rows, w_up[0], preferred_element_type=jnp.float32)
    return (jax.nn.silu(gate) * up).astype(jnp.bfloat16)


def weigh_rows(combine, returned):
    upper = combine.astype(jnp.bfloat16)
    lower = (combine - upper.astype(jnp.float32)).astype(jnp.bfloat16)
    first = jnp.dot(upper, returned, preferred_element_type=jnp.float32)
    return first + jnp.dot(lower, returned, preferred_element_type=jnp.float32)


def shards(tokens, norm_gain, routes, gate_weights, w_gate, w_up, w_down):
    values = tokens.astype(jnp.float32)
    scale = lax.rsqrt(jnp.mean(values * values, axis=-1, keepdims=True) + 1e-06)
    normed = (values * scale * norm_gain).astype(jnp.bfloat16)
    width = tokens.shape[1]
    tok_dev = tokens.shape[0]
    topk = routes.shape[1]
    experts = lax.axis_size("ep")
    capacity = min(tok_dev, max(2, 4 * tok_dev * topk // (3 * experts)))
    expert_ids = jnp.arange(experts, dtype=jnp.int32)
    hits = routes[:, :, None] == expert_ids[None, None, :]
    chosen = jnp.any(hits, axis=1).astype(jnp.int32)
    weight_tok = jnp.sum(jnp.where(hits, gate_weights[:, :, None], 0.0), axis=1)
    rank = jnp.cumsum(chosen, axis=0) - chosen
    slot = jnp.where(chosen > 0, rank * experts + expert_ids[None, :], -1)
    slot_ids = jnp.arange(capacity * experts, dtype=jnp.int32)
    placed = slot[:, :, None] == slot_ids[None, None, :]
    place = jnp.any(placed, axis=1).astype(jnp.bfloat16)
    combine = jnp.sum(jnp.where(placed, weight_tok[:, :, None], 0.0), axis=1)
    dispatch = jnp.dot(place.T, normed, preferred_element_type=jnp.float32)
    dispatch = dispatch.astype(jnp.bfloat16).reshape(capacity, experts, width)
    arrived = lax.all_to_all(dispatch, "ep", split_axis=1, concat_axis=1, tiled=True)
    rows = arrived.reshape(-1, width)
    partial_value = jnp.dot(
        hidden_rows(rows, w_gate, w_up), w_down[0], preferred_element_type=jnp.float32
    )
    output = lax.psum(partial_value.astype(jnp.bfloat16), "tp")
    returned = lax.all_to_all(
        output.reshape(arrived.shape), "ep", split_axis=1, concat_axis=1, tiled=True
    )
    mixed = weigh_rows(combine, returned.reshape(-1, width))
    return mixed.astype(jnp.bfloat16)


CORES = 2
ROWS_Y = 2
PLANE = CORES * ROWS_Y
FF_TILE = 512
D_TILE = 512


def flip(index, bits):
    bit = 1
    while bit <= bits:
        if bits & bit:
            index = index + bit - 2 * bit * lax.rem(lax.div(index, bit), 2)
        bit *= 2
    return index


def fused_kernel(
    layers, cap, tok, gain, routes, weights, wg_hbm, wu_hbm, wd_hbm, out,
    wg, wu, wd, blocks, tables, lower_tri, picked, hidden, upper_w, lower_w, parts,
    core_in, y_out, y_in, z_out, z_in,
    load_sem, own_send, fwd_send, core_fwd_send, block_in, tab_in,
    core_send, core_recv, y_send, y_recv, z_send, z_recv,
):
    me = lax.axis_index("ep")
    tokens, width = tok.shape
    topk = routes.shape[1]
    group = PLANE * tokens
    slots = PLANE * cap
    units = wg.shape[1]
    z = lax.div(me, PLANE)
    y = lax.rem(lax.div(me, CORES), ROWS_Y)
    c = lax.rem(me, CORES)

    def at(zz, yy, cc):
        return zz * PLANE + yy * CORES + cc

    oy, oc = 1 - y, 1 - c
    partner, across = at(z, y, oc), at(z, oy, c)
    far = [flip(z, k) for k in range(layers)]

    barrier = pltpu.get_barrier_semaphore()
    peers = [partner, across] + [at(far[k], y, c) for k in range(1, layers)]
    for peer in peers:
        pl.semaphore_signal(barrier, inc=1, device_id={"ep": peer})

    loads = [
        pltpu.make_async_copy(wg_hbm.at[0], wg, load_sem.at[0]),
        pltpu.make_async_copy(wu_hbm.at[0], wu, load_sem.at[1]),
        pltpu.make_async_copy(wd_hbm.at[0], wd, load_sem.at[2]),
    ]
    for load in loads:
        load.start()

    values = tok[...].astype(jnp.float32)
    scale = lax.rsqrt(jnp.mean(values * values, axis=-1, keepdims=True) + 1e-06)
    normed = (values * scale * gain[...]).astype(jnp.bfloat16)
    blocks[pl.ds(pl.multiple_of(me * tokens, tokens), tokens), :] = normed

    lane = lax.broadcasted_iota(jnp.int32, (tokens, 2 * tokens), 1)
    by_expert = jnp.zeros((tokens, 2 * tokens), jnp.float32)
    for j in range(topk):
        by_expert = by_expert + jnp.where(routes[:, j:j + 1] == lane, weights[:, j:j + 1], 0.0)
    doubled = jnp.concatenate([by_expert, by_expert], axis=0)
    half = lax.broadcasted_iota(jnp.int32, doubled.shape, 0) // tokens
    table = jnp.where(half == c, doubled, 0.0).T
    tables[me] = table[: tables.shape[1], :]

    r = lax.broadcasted_iota(jnp.int32, (group, group), 0)
    t = lax.broadcasted_iota(jnp.int32, (group, group), 1)
    before = (r < t) & (r // tokens == t // tokens)
    lower_tri[...] = jnp.where(before, 1.0, 0.0).astype(jnp.bfloat16)

    sent = []

    def push(src, dst, send_sem, recv_sem, peer):
        copy = pltpu.make_async_remote_copy(
            src_ref=src, dst_ref=dst, send_sem=send_sem, recv_sem=recv_sem,
            device_id={"ep": peer},
        )
        copy.start()
        sent.append(copy)

    def landed(dst, send_sem, recv_sem):
        pltpu.make_async_remote_copy(
            src_ref=dst, dst_ref=dst, send_sem=send_sem, recv_sem=recv_sem,
            device_id={"ep": partner},
        ).wait_recv()

    def block(slot):
        return blocks.at[pl.ds(pl.multiple_of(slot * tokens, tokens), tokens), :]

    def share(slot, peer, sems, position):
        push(tables.at[slot], tables.at[slot], sems.at[position, 1], tab_in.at[slot], peer)
        push(block(slot), block(slot), sems.at[position, 0], block_in.at[slot], peer)

    def await_share(slot):
        landed(tables.at[slot], own_send.at[0, 1], tab_in.at[slot])
        landed(block(slot), own_send.at[0, 0], block_in.at[slot])

    pl.semaphore_wait(barrier, len(peers))
    share(me, across, own_send, 0)
    for k in range(1, layers):
        share(me, at(far[k], y, c), own_send, k)
    share(me, partner, core_fwd_send, 0)

    def from_z(k):
        slot = at(far[k], y, c)
        await_share(slot)
        share(slot, across, fwd_send, k)
        share(slot, partner, core_fwd_send, k)

    def from_y(k):
        slot = at(far[k], oy, c)
        await_share(slot)
        share(slot, partner, core_fwd_send, layers + k)

    def from_core(k):
        await_share(at(far[k], y, oc))
        await_share(at(far[k], oy, oc))

    def gather(k):
        base = far[k] * PLANE
        pairs = [
            tables[base + CORES * yy, pl.ds(me, 1), :] + tables[base + CORES * yy + 1, pl.ds(me, 1), :]
            for yy in range(ROWS_Y)
        ]
        weight = jnp.broadcast_to(jnp.concatenate(pairs, axis=1), (slots, group))
        chosen = weight > 0.0
        rank = jnp.dot(
            jnp.where(chosen, 1.0, 0.0).astype(jnp.bfloat16), lower_tri[...],
            preferred_element_type=jnp.float32,
        )
        row = lax.broadcasted_iota(jnp.int32, (slots, group), 0)
        column = lax.broadcasted_iota(jnp.int32, (slots, group), 1)
        place = chosen & (rank == (row % cap).astype(jnp.float32)) & (row // cap == column // tokens)
        pick = jnp.where(place, 1.0, 0.0).astype(jnp.bfloat16)
        spread = jnp.where(place, weight, 0.0).T
        upper = spread.astype(jnp.bfloat16)
        upper_w[...] = upper
        lower_w[...] = (spread - upper.astype(jnp.float32)).astype(jnp.bfloat16)
        rows = blocks[pl.ds(pl.multiple_of(base * tokens, group), group), :]
        picked[...] = jnp.dot(pick, rows, preferred_element_type=jnp.float32).astype(jnp.bfloat16)

    def gate_up():
        @pl.loop(0, units // FF_TILE)
        def _(i):
            cols = pl.ds(pl.multiple_of(i * FF_TILE, FF_TILE), FF_TILE)
            gate = jnp.dot(picked[...], wg[:, cols], preferred_element_type=jnp.float32)
            up = jnp.dot(picked[...], wu[:, cols], preferred_element_type=jnp.float32)
            hidden[:, cols] = (gate / (1.0 + jnp.exp(-gate)) * up).astype(jnp.bfloat16)

    def down(k):
        @pl.loop(0, width // D_TILE)
        def _(i):
            cols = pl.ds(pl.multiple_of(i * D_TILE, D_TILE), D_TILE)
            expert_out = jnp.dot(
                hidden[...], wd[:, cols], preferred_element_type=jnp.float32
            ).astype(jnp.bfloat16)
            part = jnp.dot(upper_w[...], expert_out, preferred_element_type=jnp.float32)
            part = part + jnp.dot(lower_w[...], expert_out, preferred_element_type=jnp.float32)
            parts[k, :, cols] = part.astype(jnp.bfloat16)

    def part_of(k, yy, cc):
        start = pl.multiple_of((yy * CORES + cc) * tokens, tokens)
        return parts.at[k, pl.ds(start, tokens), :]

    def core_stage(k):
        for position, yy in enumerate((oy, y)):
            push(part_of(k, yy, oc), core_in.at[k, position],
                 core_send.at[k, position], core_recv.at[k, position], partner)

    def y_stage(k):
        landed(core_in.at[k, 0], core_send.at[k, 0], core_recv.at[k, 0])
        both = part_of(k, oy, c)[...].astype(jnp.float32) + core_in[k, 0].astype(jnp.float32)
        y_out[k] = both.astype(jnp.bfloat16)
        push(y_out.at[k], y_in.at[k], y_send.at[k], y_recv.at[k], across)

    def layer_sum(k):
        landed(core_in.at[k, 1], core_send.at[k, 1], core_recv.at[k, 1])
        both = part_of(k, y, c)[...].astype(jnp.float32) + core_in[k, 1].astype(jnp.float32)
        landed(y_in.at[k], y_send.at[k], y_recv.at[k])
        return both + y_in[k].astype(jnp.float32)

    def z_stage(k):
        if k == 0:
            return
        z_out[k] = layer_sum(k).astype(jnp.bfloat16)
        push(z_out.at[k], z_in.at[k], z_send.at[k], z_recv.at[k], at(far[k], y, c))

    for k in range(layers):
        from_y(k)
        from_core(k)
        gather(k)
        if k == 0:
            loads[0].wait()
            loads[1].wait()
        gate_up()
        if k + 1 < layers:
            from_z(k + 1)
        if k >= 2:
            z_stage(k - 2)
        if k >= 1:
            y_stage(k - 1)
        if k == 0:
            loads[2].wait()
        down(k)
        core_stage(k)
    if layers >= 2:
        z_stage(layers - 2)
    y_stage(layers - 1)
    total = layer_sum(0)
    z_stage(layers - 1)
    for k in range(1, layers):
        landed(z_in.at[k], z_send.at[k], z_recv.at[k])
        total = total + z_in[k].astype(jnp.float32)
    out[...] = total.astype(jnp.bfloat16)
    for copy in sent:
        copy.wait_send()


def fused_shards(tokens, norm_gain, routes, gate_weights, w_gate, w_up, w_down):
    tok_dev, width = tokens.shape
    units = w_gate.shape[2]
    topk = routes.shape[1]
    experts = lax.axis_size("ep")
    layers = experts // PLANE
    cap = min(tok_dev, max(2, 4 * tok_dev * topk // (3 * experts)))
    vmem = pl.BlockSpec(memory_space=pltpu.VMEM)
    hbm = pl.BlockSpec(memory_space=pltpu.MemorySpace.HBM)
    dma = pltpu.SemaphoreType.DMA
    bf = jnp.bfloat16
    return pl.pallas_call(
        functools.partial(fused_kernel, layers, cap),
        out_shape=jax.ShapeDtypeStruct((tok_dev, width), bf),
        in_specs=[vmem] * 4 + [hbm] * 3,
        out_specs=vmem,
        scratch_shapes=[
            pltpu.VMEM((width, units), bf),
            pltpu.VMEM((width, units), bf),
            pltpu.VMEM((units, width), bf),
            pltpu.VMEM((experts * tok_dev, width), bf),
            pltpu.VMEM((experts, experts, 2 * tok_dev), jnp.float32),
            pltpu.VMEM((PLANE * tok_dev, PLANE * tok_dev), bf),
            pltpu.VMEM((PLANE * cap, width), bf),
            pltpu.VMEM((PLANE * cap, units), bf),
            pltpu.VMEM((PLANE * tok_dev, PLANE * cap), bf),
            pltpu.VMEM((PLANE * tok_dev, PLANE * cap), bf),
            pltpu.VMEM((layers, PLANE * tok_dev, width), bf),
            pltpu.VMEM((layers, 2, tok_dev, width), bf),
            pltpu.VMEM((layers, tok_dev, width), bf),
            pltpu.VMEM((layers, tok_dev, width), bf),
            pltpu.VMEM((layers, tok_dev, width), bf),
            pltpu.VMEM((layers, tok_dev, width), bf),
            dma((3,)),
            dma((layers, 2)),
            dma((layers, 2)),
            dma((2 * layers, 2)),
            dma((experts,)),
            dma((experts,)),
            dma((layers, 2)),
            dma((layers, 2)),
            dma((layers,)),
            dma((layers,)),
            dma((layers,)),
            dma((layers,)),
        ],
        compiler_params=pltpu.CompilerParams(
            collective_id=0, has_side_effects=True, vmem_limit_bytes=48 * 1024 * 1024
        ),
    )(tokens, norm_gain.reshape(1, width), routes, gate_weights, w_gate, w_up, w_down)


def fits_fused(mesh, tokens, w_gate):
    experts = mesh.shape["ep"]
    layers = experts // PLANE
    tok_dev = tokens.shape[0] // (mesh.shape["grp"] * experts)
    return (
        mesh.shape["tp"] == 1 and experts % PLANE == 0 and layers & (layers - 1) == 0
        and tok_dev == 64 and experts % 8 == 0 and experts <= 128
        and tokens.shape[1] % D_TILE == 0 and w_gate.shape[2] % FF_TILE == 0
    )


def solution(mesh):
    in_specs = (
        P(("grp", "ep"), None),
        P(),
        P(("grp", "ep"), None),
        P(("grp", "ep"), None),
        P("ep", None, "tp"),
        P("ep", None, "tp"),
        P("ep", "tp", None),
    )
    out_specs = P(("grp", "ep"), None)

    def layer(tokens, norm_gain, routes, gate_weights, w_gate, w_up, w_down):
        body = fused_shards if fits_fused(mesh, tokens, w_gate) else shards
        return jax.shard_map(
            body, mesh=mesh, in_specs=in_specs, out_specs=out_specs, check_vma=False
        )(tokens, norm_gain, routes, gate_weights, w_gate, w_up, w_down)

    return layer
```

```python
import functools

import jax
import jax.numpy as jnp
from jax import lax
from jax.experimental import pallas as pl
from jax.experimental.pallas import tpu as pltpu
from jax.sharding import PartitionSpec as P


def hidden_rows(rows, w_gate, w_up):
    gate = jnp.dot(rows, w_gate[0], preferred_element_type=jnp.float32)
    up = jnp.dot(rows, w_up[0], preferred_element_type=jnp.float32)
    return (jax.nn.silu(gate) * up).astype(jnp.bfloat16)


def weigh_rows(combine, returned):
    upper = combine.astype(jnp.bfloat16)
    lower = (combine - upper.astype(jnp.float32)).astype(jnp.bfloat16)
    first = jnp.dot(upper, returned, preferred_element_type=jnp.float32)
    return first + jnp.dot(lower, returned, preferred_element_type=jnp.float32)


def shards(tokens, norm_gain, routes, gate_weights, w_gate, w_up, w_down):
    values = tokens.astype(jnp.float32)
    scale = lax.rsqrt(jnp.mean(values * values, axis=-1, keepdims=True) + 1e-06)
    normed = (values * scale * norm_gain).astype(jnp.bfloat16)
    width = tokens.shape[1]
    tok_dev = tokens.shape[0]
    topk = routes.shape[1]
    experts = lax.axis_size("ep")
    capacity = min(tok_dev, max(2, 4 * tok_dev * topk // (3 * experts)))
    expert_ids = jnp.arange(experts, dtype=jnp.int32)
    hits = routes[:, :, None] == expert_ids[None, None, :]
    chosen = jnp.any(hits, axis=1).astype(jnp.int32)
    weight_tok = jnp.sum(jnp.where(hits, gate_weights[:, :, None], 0.0), axis=1)
    rank = jnp.cumsum(chosen, axis=0) - chosen
    slot = jnp.where(chosen > 0, rank * experts + expert_ids[None, :], -1)
    slot_ids = jnp.arange(capacity * experts, dtype=jnp.int32)
    placed = slot[:, :, None] == slot_ids[None, None, :]
    place = jnp.any(placed, axis=1).astype(jnp.bfloat16)
    combine = jnp.sum(jnp.where(placed, weight_tok[:, :, None], 0.0), axis=1)
    dispatch = jnp.dot(place.T, normed, preferred_element_type=jnp.float32)
    dispatch = dispatch.astype(jnp.bfloat16).reshape(capacity, experts, width)
    arrived = lax.all_to_all(dispatch, "ep", split_axis=1, concat_axis=1, tiled=True)
    rows = arrived.reshape(-1, width)
    partial_value = jnp.dot(
        hidden_rows(rows, w_gate, w_up), w_down[0], preferred_element_type=jnp.float32
    )
    output = lax.psum(partial_value.astype(jnp.bfloat16), "tp")
    returned = lax.all_to_all(
        output.reshape(arrived.shape), "ep", split_axis=1, concat_axis=1, tiled=True
    )
    mixed = weigh_rows(combine, returned.reshape(-1, width))
    return mixed.astype(jnp.bfloat16)


CORES = 2
ROWS_Y = 2
PLANE = CORES * ROWS_Y
FF_TILE = 512
HALVES = 2


def near_first(index, layers):
    orders = [sorted(range(layers), key=lambda v: (abs(v - own), v)) for own in range(layers)]
    result = []
    for k in range(layers):
        value = orders[0][k]
        for own in range(1, layers):
            value = jnp.where(index == own, orders[own][k], value)
        result.append(value)
    return result


def fused_kernel(
    layers, cap, tok_hbm, gain_hbm, routes_hbm, weights_hbm, wg_hbm, wu_hbm, wd_hbm, out,
    tok, gain, routes, weights, wg, wu, wd, blocks, tables, lower_tri, picked, hidden,
    upper_w, lower_w, parts, core_in, y_out, y_in, z_out, z_in,
    load_sem, own_send, line_send, fwd_send, core_fwd_send, tab_send, block_in, tab_in,
    core_send, core_recv, y_send, y_recv, z_send, z_recv,
):
    me = lax.axis_index("ep")
    tokens, width = tok.shape
    topk = routes.shape[0]
    group = PLANE * tokens
    slots = PLANE * cap
    units = wg.shape[1]
    span = width // HALVES
    experts = tables.shape[0]
    z = lax.div(me, PLANE)
    y = lax.rem(lax.div(me, CORES), ROWS_Y)
    c = lax.rem(me, CORES)

    def at(zz, yy, cc):
        return zz * PLANE + yy * CORES + cc

    oy, oc = 1 - y, 1 - c
    partner, across = at(z, y, oc), at(z, oy, c)
    far = near_first(z, layers)

    barrier = pltpu.get_barrier_semaphore()
    peers = [partner, across] + [at(far[k], y, c) for k in range(1, layers)]
    for peer in peers:
        pl.semaphore_signal(barrier, inc=1, device_id={"ep": peer})

    small = [
        pltpu.make_async_copy(tok_hbm, tok, load_sem.at[3]),
        pltpu.make_async_copy(gain_hbm, gain, load_sem.at[4]),
        pltpu.make_async_copy(routes_hbm, routes, load_sem.at[5]),
        pltpu.make_async_copy(weights_hbm, weights, load_sem.at[6]),
    ]
    loads = [
        pltpu.make_async_copy(wg_hbm.at[0], wg, load_sem.at[0]),
        pltpu.make_async_copy(wu_hbm.at[0], wu, load_sem.at[1]),
        pltpu.make_async_copy(wd_hbm.at[0], wd, load_sem.at[2]),
    ]
    for load in small + loads:
        load.start()

    r = lax.broadcasted_iota(jnp.int32, (group, group), 0)
    t = lax.broadcasted_iota(jnp.int32, (group, group), 1)
    before = (r < t) & (r // tokens == t // tokens)
    lower_tri[...] = jnp.where(before, 1.0, 0.0).astype(jnp.bfloat16)

    for load in small:
        load.wait()
    values = tok[...].astype(jnp.float32)
    scale = lax.rsqrt(jnp.mean(values * values, axis=-1, keepdims=True) + 1e-06)
    normed = (values * scale * gain[...]).astype(jnp.bfloat16)
    own_rows = pl.ds(pl.multiple_of(me * tokens, tokens), tokens)
    for h in range(HALVES):
        blocks[h, own_rows, :] = normed[:, h * span:(h + 1) * span]

    expert_id = lax.broadcasted_iota(jnp.int32, (experts, tokens), 0)
    table = jnp.zeros((experts, tokens), jnp.float32)
    for j in range(topk):
        table = table + jnp.where(routes[j:j + 1, :] == expert_id, weights[j:j + 1, :], 0.0)
    doubled = jnp.concatenate([table, table], axis=1)
    half = lax.broadcasted_iota(jnp.int32, doubled.shape, 1) // tokens
    tables[me] = jnp.where(half == c, doubled, 0.0)

    sent = []

    def push(src, dst, send_sem, recv_sem, peer, when=None):
        copy = pltpu.make_async_remote_copy(
            src_ref=src, dst_ref=dst, send_sem=send_sem, recv_sem=recv_sem,
            device_id={"ep": peer},
        )
        if when is None:
            copy.start()
        else:
            pl.when(when)(copy.start)
        sent.append((copy, when))

    def landed(dst, send_sem, recv_sem):
        pltpu.make_async_remote_copy(
            src_ref=dst, dst_ref=dst, send_sem=send_sem, recv_sem=recv_sem,
            device_id={"ep": partner},
        ).wait_recv()

    def block(h, slot):
        return blocks.at[h, pl.ds(pl.multiple_of(slot * tokens, tokens), tokens), :]

    counter = [0]

    def share(h, slot, peer, sem, when=None):
        if h == 0:
            position = counter[0]
            counter[0] += 1
            push(tables.at[slot], tables.at[slot], tab_send.at[position], tab_in.at[slot], peer, when)
        push(block(h, slot), block(h, slot), sem, block_in.at[slot, h], peer, when)

    def await_share(h, slot):
        if h == 0:
            landed(tables.at[slot], tab_send.at[0], tab_in.at[slot])
        landed(block(h, slot), own_send.at[0, h], block_in.at[slot, h])

    pl.semaphore_wait(barrier, len(peers))
    for h in range(HALVES):
        share(h, me, across, own_send.at[0, h])
        share(h, me, at(lax.rem(z + 1, layers), y, c), own_send.at[1, h], z + 1 < layers)
        share(h, me, at(lax.rem(z + layers - 1, layers), y, c), own_send.at[2, h], z > 0)
    for h in range(HALVES):
        share(h, me, partner, core_fwd_send.at[0, h])

    def from_z(k):
        slot = at(far[k], y, c)
        step = jnp.where(far[k] < z, 1, -1)
        inside = (z + step >= 0) & (z + step < layers)
        onward = at(lax.rem(z + step + layers, layers), y, c)
        for h in range(HALVES):
            await_share(h, slot)
            share(h, slot, onward, line_send.at[k, h], inside)
            share(h, slot, across, fwd_send.at[k, h])
            share(h, slot, partner, core_fwd_send.at[k, h])

    def from_y(k):
        slot = at(far[k], oy, c)
        for h in range(HALVES):
            await_share(h, slot)
            share(h, slot, partner, core_fwd_send.at[layers + k, h])

    def from_core(k):
        for h in range(HALVES):
            await_share(h, at(far[k], y, oc))
            await_share(h, at(far[k], oy, oc))

    def gather(k):
        base = far[k] * PLANE
        pairs = [
            tables[base + CORES * yy, pl.ds(me, 1), :] + tables[base + CORES * yy + 1, pl.ds(me, 1), :]
            for yy in range(ROWS_Y)
        ]
        weight = jnp.broadcast_to(jnp.concatenate(pairs, axis=1), (slots, group))
        chosen = weight > 0.0
        rank = jnp.dot(
            jnp.where(chosen, 1.0, 0.0).astype(jnp.bfloat16), lower_tri[...],
            preferred_element_type=jnp.float32,
        )
        row = lax.broadcasted_iota(jnp.int32, (slots, group), 0)
        column = lax.broadcasted_iota(jnp.int32, (slots, group), 1)
        place = chosen & (rank == (row % cap).astype(jnp.float32)) & (row // cap == column // tokens)
        pick = jnp.where(place, 1.0, 0.0).astype(jnp.bfloat16)
        spread = jnp.where(place, weight, 0.0).T
        upper = spread.astype(jnp.bfloat16)
        upper_w[...] = upper
        lower_w[...] = (spread - upper.astype(jnp.float32)).astype(jnp.bfloat16)
        for h in range(HALVES):
            rows = blocks[h, pl.ds(pl.multiple_of(base * tokens, group), group), :]
            found = jnp.dot(pick, rows, preferred_element_type=jnp.float32)
            picked[:, h * span:(h + 1) * span] = found.astype(jnp.bfloat16)

    def gate_up():
        @pl.loop(0, units // FF_TILE)
        def _(i):
            cols = pl.ds(pl.multiple_of(i * FF_TILE, FF_TILE), FF_TILE)
            gate = jnp.dot(picked[...], wg[:, cols], preferred_element_type=jnp.float32)
            up = jnp.dot(picked[...], wu[:, cols], preferred_element_type=jnp.float32)
            hidden[:, cols] = (gate / (1.0 + jnp.exp(-gate)) * up).astype(jnp.bfloat16)

    def part_of(k, h, yy, cc):
        start = pl.multiple_of((yy * CORES + cc) * tokens, tokens)
        return parts.at[k, h, pl.ds(start, tokens), :]

    def down(k):
        for h in range(HALVES):
            expert_out = jnp.dot(
                hidden[...], wd[:, h * span:(h + 1) * span], preferred_element_type=jnp.float32
            ).astype(jnp.bfloat16)
            part = jnp.dot(upper_w[...], expert_out, preferred_element_type=jnp.float32)
            part = part + jnp.dot(lower_w[...], expert_out, preferred_element_type=jnp.float32)
            parts[k, h] = part.astype(jnp.bfloat16)
            for position, yy in enumerate((oy, y)):
                push(part_of(k, h, yy, oc), core_in.at[k, h, position],
                     core_send.at[k, h, position], core_recv.at[k, h, position], partner)

    def y_stage(k):
        for h in range(HALVES):
            landed(core_in.at[k, h, 0], core_send.at[k, h, 0], core_recv.at[k, h, 0])
            both = part_of(k, h, oy, c)[...].astype(jnp.float32) + core_in[k, h, 0].astype(jnp.float32)
            y_out[k, h] = both.astype(jnp.bfloat16)
            push(y_out.at[k, h], y_in.at[k, h], y_send.at[k, h], y_recv.at[k, h], across)

    def layer_sum(k, h):
        landed(core_in.at[k, h, 1], core_send.at[k, h, 1], core_recv.at[k, h, 1])
        both = part_of(k, h, y, c)[...].astype(jnp.float32) + core_in[k, h, 1].astype(jnp.float32)
        landed(y_in.at[k, h], y_send.at[k, h], y_recv.at[k, h])
        return both + y_in[k, h].astype(jnp.float32)

    def z_stage(k):
        for h in range(HALVES):
            z_out[k, h] = layer_sum(k, h).astype(jnp.bfloat16)
            push(z_out.at[k, h], z_in.at[z, h], z_send.at[k, h], z_recv.at[z, h], at(far[k], y, c))

    last = layers - 1
    if last >= 1:
        from_z(1)
    for k in range(layers):
        from_y(k)
        if k == 1:
            for ahead in range(3, layers):
                from_z(ahead)
        from_core(k)
        gather(k)
        if k == 0:
            loads[0].wait()
            loads[1].wait()
        gate_up()
        if k == 0:
            if last >= 2:
                from_z(2)
            loads[2].wait()
        if k >= 3:
            z_stage(k - 2)
        if k >= 1:
            y_stage(k - 1)
        down(k)
    if last >= 2:
        z_stage(last - 1)
    y_stage(last)
    totals = [layer_sum(0, h) for h in range(HALVES)]
    if last >= 1:
        z_stage(last)
    for h in range(HALVES):
        total = totals[h]
        for k in range(1, layers):
            landed(z_in.at[far[k], h], z_send.at[k, h], z_recv.at[far[k], h])
            total = total + z_in[far[k], h].astype(jnp.float32)
        out[:, h * span:(h + 1) * span] = total.astype(jnp.bfloat16)
    for copy, when in sent:
        if when is None:
            copy.wait_send()
        else:
            pl.when(when)(copy.wait_send)


def fused_shards(tokens, norm_gain, routes, gate_weights, w_gate, w_up, w_down):
    tok_dev, width = tokens.shape
    units = w_gate.shape[2]
    topk = routes.shape[1]
    experts = lax.axis_size("ep")
    layers = experts // PLANE
    cap = min(tok_dev, max(2, 4 * tok_dev * topk // (3 * experts)))
    vmem = pl.BlockSpec(memory_space=pltpu.VMEM)
    hbm = pl.BlockSpec(memory_space=pltpu.MemorySpace.HBM)
    dma = pltpu.SemaphoreType.DMA
    bf = jnp.bfloat16
    span = width // HALVES
    return pl.pallas_call(
        functools.partial(fused_kernel, layers, cap),
        out_shape=jax.ShapeDtypeStruct((tok_dev, width), bf),
        in_specs=[hbm] * 7,
        out_specs=vmem,
        scratch_shapes=[
            pltpu.VMEM((tok_dev, width), bf),
            pltpu.VMEM((1, width), jnp.float32),
            pltpu.VMEM((topk, tok_dev), jnp.int32),
            pltpu.VMEM((topk, tok_dev), jnp.float32),
            pltpu.VMEM((width, units), bf),
            pltpu.VMEM((width, units), bf),
            pltpu.VMEM((units, width), bf),
            pltpu.VMEM((HALVES, experts * tok_dev, span), bf),
            pltpu.VMEM((experts, experts, 2 * tok_dev), jnp.float32),
            pltpu.VMEM((PLANE * tok_dev, PLANE * tok_dev), bf),
            pltpu.VMEM((PLANE * cap, width), bf),
            pltpu.VMEM((PLANE * cap, units), bf),
            pltpu.VMEM((PLANE * tok_dev, PLANE * cap), bf),
            pltpu.VMEM((PLANE * tok_dev, PLANE * cap), bf),
            pltpu.VMEM((layers, HALVES, PLANE * tok_dev, span), bf),
            pltpu.VMEM((layers, HALVES, 2, tok_dev, span), bf),
            pltpu.VMEM((layers, HALVES, tok_dev, span), bf),
            pltpu.VMEM((layers, HALVES, tok_dev, span), bf),
            pltpu.VMEM((layers, HALVES, tok_dev, span), bf),
            pltpu.VMEM((layers, HALVES, tok_dev, span), bf),
            dma((7,)),
            dma((3, HALVES)),
            dma((layers, HALVES)),
            dma((layers, HALVES)),
            dma((2 * layers, HALVES)),
            dma((5 * layers,)),
            dma((experts, HALVES)),
            dma((experts,)),
            dma((layers, HALVES, 2)),
            dma((layers, HALVES, 2)),
            dma((layers, HALVES)),
            dma((layers, HALVES)),
            dma((layers, HALVES)),
            dma((layers, HALVES)),
        ],
        compiler_params=pltpu.CompilerParams(
            collective_id=0, has_side_effects=True, vmem_limit_bytes=60 * 1024 * 1024
        ),
    )(tokens, norm_gain.reshape(1, width), routes.T, gate_weights.T, w_gate, w_up, w_down)


def fits_fused(mesh, tokens, w_gate):
    experts = mesh.shape["ep"]
    layers = experts // PLANE
    tok_dev = tokens.shape[0] // (mesh.shape["grp"] * experts)
    return (
        mesh.shape["tp"] == 1 and experts % PLANE == 0 and layers & (layers - 1) == 0
        and tok_dev == 64 and experts % 8 == 0 and experts <= 128
        and tokens.shape[1] % (128 * HALVES) == 0 and w_gate.shape[2] % FF_TILE == 0
    )


def solution(mesh):
    in_specs = (
        P(("grp", "ep"), None),
        P(),
        P(("grp", "ep"), None),
        P(("grp", "ep"), None),
        P("ep", None, "tp"),
        P("ep", None, "tp"),
        P("ep", "tp", None),
    )
    out_specs = P(("grp", "ep"), None)

    def layer(tokens, norm_gain, routes, gate_weights, w_gate, w_up, w_down):
        body = fused_shards if fits_fused(mesh, tokens, w_gate) else shards
        return jax.shard_map(
            body, mesh=mesh, in_specs=in_specs, out_specs=out_specs, check_vma=False
        )(tokens, norm_gain, routes, gate_weights, w_gate, w_up, w_down)

    return layer
```

```python
import functools

import jax
import jax.numpy as jnp
from jax import lax
from jax.experimental import pallas as pl
from jax.experimental.pallas import tpu as pltpu
from jax.sharding import PartitionSpec as P


def hidden_rows(rows, w_gate, w_up):
    gate = jnp.dot(rows, w_gate[0], preferred_element_type=jnp.float32)
    up = jnp.dot(rows, w_up[0], preferred_element_type=jnp.float32)
    return (jax.nn.silu(gate) * up).astype(jnp.bfloat16)


def weigh_rows(combine, returned):
    upper = combine.astype(jnp.bfloat16)
    lower = (combine - upper.astype(jnp.float32)).astype(jnp.bfloat16)
    first = jnp.dot(upper, returned, preferred_element_type=jnp.float32)
    return first + jnp.dot(lower, returned, preferred_element_type=jnp.float32)


def shards(tokens, norm_gain, routes, gate_weights, w_gate, w_up, w_down):
    values = tokens.astype(jnp.float32)
    scale = lax.rsqrt(jnp.mean(values * values, axis=-1, keepdims=True) + 1e-06)
    normed = (values * scale * norm_gain).astype(jnp.bfloat16)
    width = tokens.shape[1]
    tok_dev = tokens.shape[0]
    topk = routes.shape[1]
    experts = lax.axis_size("ep")
    capacity = min(tok_dev, max(2, 4 * tok_dev * topk // (3 * experts)))
    expert_ids = jnp.arange(experts, dtype=jnp.int32)
    hits = routes[:, :, None] == expert_ids[None, None, :]
    chosen = jnp.any(hits, axis=1).astype(jnp.int32)
    weight_tok = jnp.sum(jnp.where(hits, gate_weights[:, :, None], 0.0), axis=1)
    rank = jnp.cumsum(chosen, axis=0) - chosen
    slot = jnp.where(chosen > 0, rank * experts + expert_ids[None, :], -1)
    slot_ids = jnp.arange(capacity * experts, dtype=jnp.int32)
    placed = slot[:, :, None] == slot_ids[None, None, :]
    place = jnp.any(placed, axis=1).astype(jnp.bfloat16)
    combine = jnp.sum(jnp.where(placed, weight_tok[:, :, None], 0.0), axis=1)
    dispatch = jnp.dot(place.T, normed, preferred_element_type=jnp.float32)
    dispatch = dispatch.astype(jnp.bfloat16).reshape(capacity, experts, width)
    arrived = lax.all_to_all(dispatch, "ep", split_axis=1, concat_axis=1, tiled=True)
    rows = arrived.reshape(-1, width)
    partial_value = jnp.dot(
        hidden_rows(rows, w_gate, w_up), w_down[0], preferred_element_type=jnp.float32
    )
    output = lax.psum(partial_value.astype(jnp.bfloat16), "tp")
    returned = lax.all_to_all(
        output.reshape(arrived.shape), "ep", split_axis=1, concat_axis=1, tiled=True
    )
    mixed = weigh_rows(combine, returned.reshape(-1, width))
    return mixed.astype(jnp.bfloat16)


CORES = 2
ROWS_Y = 2
PLANE = CORES * ROWS_Y
FF_TILE = 2048
HALVES = 2


def near_first(index, layers):
    orders = [sorted(range(layers), key=lambda v: (abs(v - own), v)) for own in range(layers)]
    result = []
    for k in range(layers):
        value = orders[0][k]
        for own in range(1, layers):
            value = jnp.where(index == own, orders[own][k], value)
        result.append(value)
    return result


def fused_kernel(
    layers, cap, tok_hbm, gain_hbm, routes_hbm, weights_hbm, wg_hbm, wu_hbm, wd_hbm, out,
    tok, gain, routes, weights, wg, wu, wd, blocks, tables, lower_tri, picked, hidden,
    upper_w, lower_w, parts, core_in, y_out, y_in, z_out, z_in,
    load_sem, own_send, line_send, fwd_send, core_fwd_send, tab_send, block_in, tab_in,
    core_send, core_recv, y_send, y_recv, z_send, z_recv,
):
    me = lax.axis_index("ep")
    tokens, width = tok.shape
    topk = routes.shape[0]
    group = PLANE * tokens
    slots = PLANE * cap
    units = wg.shape[1]
    span = width // HALVES
    experts = tables.shape[0]
    z = lax.div(me, PLANE)
    y = lax.rem(lax.div(me, CORES), ROWS_Y)
    c = lax.rem(me, CORES)

    def at(zz, yy, cc):
        return zz * PLANE + yy * CORES + cc

    oy, oc = 1 - y, 1 - c
    partner, across = at(z, y, oc), at(z, oy, c)
    far = near_first(z, layers)

    barrier = pltpu.get_barrier_semaphore()
    peers = [partner, across] + [at(far[k], y, c) for k in range(1, layers)]
    for peer in peers:
        pl.semaphore_signal(barrier, inc=1, device_id={"ep": peer})

    small = [
        pltpu.make_async_copy(tok_hbm, tok, load_sem.at[3]),
        pltpu.make_async_copy(gain_hbm, gain, load_sem.at[4]),
        pltpu.make_async_copy(routes_hbm, routes, load_sem.at[5]),
        pltpu.make_async_copy(weights_hbm, weights, load_sem.at[6]),
    ]
    loads = [
        pltpu.make_async_copy(wg_hbm.at[0], wg, load_sem.at[0]),
        pltpu.make_async_copy(wu_hbm.at[0], wu, load_sem.at[1]),
        pltpu.make_async_copy(wd_hbm.at[0], wd, load_sem.at[2]),
    ]
    for load in small + loads:
        load.start()

    r = lax.broadcasted_iota(jnp.int32, (group, group), 0)
    t = lax.broadcasted_iota(jnp.int32, (group, group), 1)
    before = (r < t) & (r // tokens == t // tokens)
    lower_tri[...] = jnp.where(before, 1.0, 0.0).astype(jnp.bfloat16)

    for load in small:
        load.wait()
    values = tok[...].astype(jnp.float32)
    scale = lax.rsqrt(jnp.mean(values * values, axis=-1, keepdims=True) + 1e-06)
    normed = (values * scale * gain[...]).astype(jnp.bfloat16)
    own_rows = pl.ds(pl.multiple_of(me * tokens, tokens), tokens)
    for h in range(HALVES):
        blocks[h, own_rows, :] = normed[:, h * span:(h + 1) * span]

    expert_id = lax.broadcasted_iota(jnp.int32, (experts, tokens), 0)
    table = jnp.zeros((experts, tokens), jnp.float32)
    for j in range(topk):
        table = table + jnp.where(routes[j:j + 1, :] == expert_id, weights[j:j + 1, :], 0.0)
    doubled = jnp.concatenate([table, table], axis=1)
    half = lax.broadcasted_iota(jnp.int32, doubled.shape, 1) // tokens
    tables[me] = jnp.where(half == c, doubled, 0.0)

    sent = []

    def push(src, dst, send_sem, recv_sem, peer, when=None):
        copy = pltpu.make_async_remote_copy(
            src_ref=src, dst_ref=dst, send_sem=send_sem, recv_sem=recv_sem,
            device_id={"ep": peer},
        )
        if when is None:
            copy.start()
        else:
            pl.when(when)(copy.start)
        sent.append((copy, when))

    def landed(dst, send_sem, recv_sem):
        pltpu.make_async_remote_copy(
            src_ref=dst, dst_ref=dst, send_sem=send_sem, recv_sem=recv_sem,
            device_id={"ep": partner},
        ).wait_recv()

    def block(h, slot):
        return blocks.at[h, pl.ds(pl.multiple_of(slot * tokens, tokens), tokens), :]

    counter = [0]

    def share(h, slot, peer, sem, when=None):
        if h == 0:
            position = counter[0]
            counter[0] += 1
            push(tables.at[slot], tables.at[slot], tab_send.at[position], tab_in.at[slot], peer, when)
        push(block(h, slot), block(h, slot), sem, block_in.at[slot, h], peer, when)

    def await_share(h, slot):
        if h == 0:
            landed(tables.at[slot], tab_send.at[0], tab_in.at[slot])
        landed(block(h, slot), own_send.at[0, h], block_in.at[slot, h])

    pl.semaphore_wait(barrier, len(peers))
    for h in range(HALVES):
        share(h, me, across, own_send.at[0, h])
        share(h, me, at(lax.rem(z + 1, layers), y, c), own_send.at[1, h], z + 1 < layers)
        share(h, me, at(lax.rem(z + layers - 1, layers), y, c), own_send.at[2, h], z > 0)
    for h in range(HALVES):
        share(h, me, partner, core_fwd_send.at[0, h])

    def from_z(k):
        slot = at(far[k], y, c)
        step = jnp.where(far[k] < z, 1, -1)
        inside = (z + step >= 0) & (z + step < layers)
        onward = at(lax.rem(z + step + layers, layers), y, c)
        for h in range(HALVES):
            await_share(h, slot)
            share(h, slot, onward, line_send.at[k, h], inside)
            share(h, slot, across, fwd_send.at[k, h])
            share(h, slot, partner, core_fwd_send.at[k, h])

    def from_y(k):
        slot = at(far[k], oy, c)
        for h in range(HALVES):
            await_share(h, slot)
            share(h, slot, partner, core_fwd_send.at[layers + k, h])

    def from_core(k):
        for h in range(HALVES):
            await_share(h, at(far[k], y, oc))
            await_share(h, at(far[k], oy, oc))

    def gather(k):
        base = far[k] * PLANE
        pairs = [
            tables[base + CORES * yy, pl.ds(me, 1), :] + tables[base + CORES * yy + 1, pl.ds(me, 1), :]
            for yy in range(ROWS_Y)
        ]
        weight = jnp.broadcast_to(jnp.concatenate(pairs, axis=1), (slots, group))
        chosen = weight > 0.0
        rank = jnp.dot(
            jnp.where(chosen, 1.0, 0.0).astype(jnp.bfloat16), lower_tri[...],
            preferred_element_type=jnp.float32,
        )
        row = lax.broadcasted_iota(jnp.int32, (slots, group), 0)
        column = lax.broadcasted_iota(jnp.int32, (slots, group), 1)
        place = chosen & (rank == (row % cap).astype(jnp.float32)) & (row // cap == column // tokens)
        pick = jnp.where(place, 1.0, 0.0).astype(jnp.bfloat16)
        spread = jnp.where(place, weight, 0.0).T
        upper = spread.astype(jnp.bfloat16)
        upper_w[...] = upper
        lower_w[...] = (spread - upper.astype(jnp.float32)).astype(jnp.bfloat16)
        for h in range(HALVES):
            rows = blocks[h, pl.ds(pl.multiple_of(base * tokens, group), group), :]
            found = jnp.dot(pick, rows, preferred_element_type=jnp.float32)
            picked[:, h * span:(h + 1) * span] = found.astype(jnp.bfloat16)

    def gate_up():
        @pl.loop(0, units // FF_TILE)
        def _(i):
            cols = pl.ds(pl.multiple_of(i * FF_TILE, FF_TILE), FF_TILE)
            gate = jnp.dot(picked[...], wg[:, cols], preferred_element_type=jnp.float32)
            up = jnp.dot(picked[...], wu[:, cols], preferred_element_type=jnp.float32)
            hidden[:, cols] = (gate / (1.0 + jnp.exp(-gate)) * up).astype(jnp.bfloat16)

    def part_of(k, h, yy, cc):
        start = pl.multiple_of((yy * CORES + cc) * tokens, tokens)
        return parts.at[k, h, pl.ds(start, tokens), :]

    def down(k):
        for h in range(HALVES):
            expert_out = jnp.dot(
                hidden[...], wd[:, h * span:(h + 1) * span], preferred_element_type=jnp.float32
            ).astype(jnp.bfloat16)
            part = jnp.dot(upper_w[...], expert_out, preferred_element_type=jnp.float32)
            part = part + jnp.dot(lower_w[...], expert_out, preferred_element_type=jnp.float32)
            parts[k, h] = part.astype(jnp.bfloat16)
            for position, yy in enumerate((oy, y)):
                push(part_of(k, h, yy, oc), core_in.at[k, h, position],
                     core_send.at[k, h, position], core_recv.at[k, h, position], partner)

    def y_stage(k):
        for h in range(HALVES):
            landed(core_in.at[k, h, 0], core_send.at[k, h, 0], core_recv.at[k, h, 0])
            both = part_of(k, h, oy, c)[...].astype(jnp.float32) + core_in[k, h, 0].astype(jnp.float32)
            y_out[k, h] = both.astype(jnp.bfloat16)
            push(y_out.at[k, h], y_in.at[k, h], y_send.at[k, h], y_recv.at[k, h], across)

    def layer_sum(k, h):
        landed(core_in.at[k, h, 1], core_send.at[k, h, 1], core_recv.at[k, h, 1])
        both = part_of(k, h, y, c)[...].astype(jnp.float32) + core_in[k, h, 1].astype(jnp.float32)
        landed(y_in.at[k, h], y_send.at[k, h], y_recv.at[k, h])
        return both + y_in[k, h].astype(jnp.float32)

    def z_stage(k):
        for h in range(HALVES):
            z_out[k, h] = layer_sum(k, h).astype(jnp.bfloat16)
            push(z_out.at[k, h], z_in.at[z, h], z_send.at[k, h], z_recv.at[z, h], at(far[k], y, c))

    last = layers - 1
    if last >= 1:
        from_z(1)
    for k in range(layers):
        from_y(k)
        if k == 1:
            for ahead in range(3, layers):
                from_z(ahead)
        from_core(k)
        gather(k)
        if k == 0:
            loads[0].wait()
            loads[1].wait()
        gate_up()
        if k == 0:
            if last >= 2:
                from_z(2)
            loads[2].wait()
        if k == 1:
            y_stage(0)
        if k == last and k >= 2:
            z_stage(k - 1)
        down(k)
        if k >= 1 or last == 0:
            y_stage(k)
        if 2 <= k < last:
            z_stage(k - 1)
    totals = [layer_sum(0, h) for h in range(HALVES)]
    if last >= 1:
        z_stage(last)
    for h in range(HALVES):
        total = totals[h]
        for k in range(1, layers):
            landed(z_in.at[far[k], h], z_send.at[k, h], z_recv.at[far[k], h])
            total = total + z_in[far[k], h].astype(jnp.float32)
        out[:, h * span:(h + 1) * span] = total.astype(jnp.bfloat16)
    for copy, when in sent:
        if when is None:
            copy.wait_send()
        else:
            pl.when(when)(copy.wait_send)


def fused_shards(tokens, norm_gain, routes, gate_weights, w_gate, w_up, w_down):
    tok_dev, width = tokens.shape
    units = w_gate.shape[2]
    topk = routes.shape[1]
    experts = lax.axis_size("ep")
    layers = experts // PLANE
    cap = min(tok_dev, max(2, 4 * tok_dev * topk // (3 * experts)))
    vmem = pl.BlockSpec(memory_space=pltpu.VMEM)
    hbm = pl.BlockSpec(memory_space=pltpu.MemorySpace.HBM)
    dma = pltpu.SemaphoreType.DMA
    bf = jnp.bfloat16
    span = width // HALVES
    return pl.pallas_call(
        functools.partial(fused_kernel, layers, cap),
        out_shape=jax.ShapeDtypeStruct((tok_dev, width), bf),
        in_specs=[hbm] * 7,
        out_specs=vmem,
        scratch_shapes=[
            pltpu.VMEM((tok_dev, width), bf),
            pltpu.VMEM((1, width), jnp.float32),
            pltpu.VMEM((topk, tok_dev), jnp.int32),
            pltpu.VMEM((topk, tok_dev), jnp.float32),
            pltpu.VMEM((width, units), bf),
            pltpu.VMEM((width, units), bf),
            pltpu.VMEM((units, width), bf),
            pltpu.VMEM((HALVES, experts * tok_dev, span), bf),
            pltpu.VMEM((experts, experts, 2 * tok_dev), jnp.float32),
            pltpu.VMEM((PLANE * tok_dev, PLANE * tok_dev), bf),
            pltpu.VMEM((PLANE * cap, width), bf),
            pltpu.VMEM((PLANE * cap, units), bf),
            pltpu.VMEM((PLANE * tok_dev, PLANE * cap), bf),
            pltpu.VMEM((PLANE * tok_dev, PLANE * cap), bf),
            pltpu.VMEM((layers, HALVES, PLANE * tok_dev, span), bf),
            pltpu.VMEM((layers, HALVES, 2, tok_dev, span), bf),
            pltpu.VMEM((layers, HALVES, tok_dev, span), bf),
            pltpu.VMEM((layers, HALVES, tok_dev, span), bf),
            pltpu.VMEM((layers, HALVES, tok_dev, span), bf),
            pltpu.VMEM((layers, HALVES, tok_dev, span), bf),
            dma((7,)),
            dma((3, HALVES)),
            dma((layers, HALVES)),
            dma((layers, HALVES)),
            dma((2 * layers, HALVES)),
            dma((5 * layers,)),
            dma((experts, HALVES)),
            dma((experts,)),
            dma((layers, HALVES, 2)),
            dma((layers, HALVES, 2)),
            dma((layers, HALVES)),
            dma((layers, HALVES)),
            dma((layers, HALVES)),
            dma((layers, HALVES)),
        ],
        compiler_params=pltpu.CompilerParams(
            collective_id=0, has_side_effects=True, vmem_limit_bytes=60 * 1024 * 1024
        ),
    )(tokens, norm_gain.reshape(1, width), routes.T, gate_weights.T, w_gate, w_up, w_down)


def fits_fused(mesh, tokens, w_gate):
    experts = mesh.shape["ep"]
    layers = experts // PLANE
    tok_dev = tokens.shape[0] // (mesh.shape["grp"] * experts)
    return (
        mesh.shape["tp"] == 1 and experts % PLANE == 0 and layers & (layers - 1) == 0
        and tok_dev == 64 and experts % 8 == 0 and experts <= 128
        and tokens.shape[1] % (128 * HALVES) == 0 and w_gate.shape[2] % FF_TILE == 0
    )


def solution(mesh):
    in_specs = (
        P(("grp", "ep"), None),
        P(),
        P(("grp", "ep"), None),
        P(("grp", "ep"), None),
        P("ep", None, "tp"),
        P("ep", None, "tp"),
        P("ep", "tp", None),
    )
    out_specs = P(("grp", "ep"), None)

    def layer(tokens, norm_gain, routes, gate_weights, w_gate, w_up, w_down):
        body = fused_shards if fits_fused(mesh, tokens, w_gate) else shards
        return jax.shard_map(
            body, mesh=mesh, in_specs=in_specs, out_specs=out_specs, check_vma=False
        )(tokens, norm_gain, routes, gate_weights, w_gate, w_up, w_down)

    return layer
```
